256 devices in a mesh: sp: 32 (over z, y), tp: 8 (over x, core).
Axes of the slice: x: 4, y: 4, z: 8, core: 2. Of those that a mesh axis runs over, the one named last changes fastest.
Arguments:
- tokens: bfloat16 [24576, 4096], P('sp', 'tp'), may hold values from -6 to 6
- in_proj: bfloat16 [3, 4096, 1024], P(None, 'tp', 'sp'), may hold values from -0.09375 to 0.09375
- group_mix: bfloat16 [3, 4, 256, 256], replicated, may hold values from -0.375 to 0.375
- pool_gain: float32 [3, 1024], replicated, may hold values from 0.1 to 1.9
- out_proj: bfloat16 [3, 1024, 4096], P(None, 'sp', 'tp'), may hold values from -0.1875 to 0.1875
- norm_gain: float32 [3, 4096], P(None, 'tp'), may hold values from 0.25 to 3
- norm_bias: float32 [3, 4096], P(None, 'tp'), may hold values from -1.5 to 1.5
Outputs:
- stream_out: bfloat16 [24576, 4096], P('sp', 'tp')
The draws below stay inside these ranges and needn't reach their ends.
All inputs are finite; a program needn't handle non-finite values.
Results may differ from the reference program's by a relative error of at most 0.017.
Values may be sent and summed in bfloat16 or wider, within the bound.
No kernel may reach another device: no remote copies, remote signals or barrier semaphores. Data moves between devices by JAX's collectives and lax.ppermute only.
A program may use at most 128 MiB of HBM per device.

```python
import jax
import jax.numpy as jnp
from jax import lax

D = 4096
P_SIZE = 1024
POOL_CH = 256
LAYERS = 3
SEQ = 24576
N_TP = 8


def draw_norm_gain(key, part):
    key_block, key_noise = jax.random.split(jax.random.fold_in(key, 17))
    block_scale = jnp.exp(jax.random.uniform(key_block, (LAYERS, 8, 1), jnp.float32, -0.7, 0.7))
    noise = 0.18 * jnp.clip(jax.random.normal(key_noise, (LAYERS, 8, D // 8), jnp.float32), -2.5, 2.5)
    return (block_scale * (1.0 + noise)).reshape(LAYERS, D)


def levels(key, dims, cuts, low, top_value):
    def one(dim, parts):
        steps = jax.random.uniform(jax.random.fold_in(jax.random.fold_in(key, 6), dim), (parts,), jnp.float32, low / len(cuts), top_value / len(cuts))
        return jnp.repeat(jnp.exp(steps), dims[dim] // parts).reshape((-1,) + (1,) * (len(dims) - dim - 1))

    loudness = one(*cuts[0])
    for cut in cuts[1:]:
        loudness = loudness * one(*cut)
    return loudness


def normal_values(key, shape, deviation, reach, shards=(), kind=jnp.bfloat16):
    entries = jax.random.normal(key, shape, jnp.float32) * deviation
    if len(shards) > 0:
        entries = levels(key, shape, shards, -0.22, 0.18) * entries
    return jnp.clip(entries, min=-reach, max=reach).astype(kind)


def setup_inputs(seed: int = 0) -> dict:
    arg_keys = jax.random.split(jax.random.key(seed), 8)
    return {
        "tokens": normal_values(arg_keys[0], (SEQ, D), 1.0, 6.0, ((0, 32), (1, 8))),
        "in_proj": normal_values(arg_keys[1], (LAYERS, D, P_SIZE), D ** -0.5, 0.09375, ((1, 8), (2, 32))),
        "group_mix": normal_values(arg_keys[2], (LAYERS, 4, POOL_CH, POOL_CH), POOL_CH ** -0.5, 0.375),
        "pool_gain": jnp.clip(1.0 + 0.18 * jax.random.normal(arg_keys[3], (LAYERS, P_SIZE), jnp.float32), 0.1, 1.9),
        "out_proj": normal_values(arg_keys[4], (LAYERS, P_SIZE, D), P_SIZE ** -0.5, 0.1875, ((1, 32), (2, 8))),
        "norm_gain": draw_norm_gain(jax.random.fold_in(arg_keys[7], 71), 0),
        "norm_bias": normal_values(arg_keys[6], (LAYERS, D), 0.3, 1.5, ((1, 8),), jnp.float32),
    }


pool_windows = (2, 4, 8, 16)
norm_eps = 1e-05

def reference(tokens, in_proj, group_mix, pool_gain, out_proj, norm_gain, norm_bias):
    residual_scale = (2.0 * LAYERS) ** 0.25
    stream = tokens
    seq_length = stream.shape[0]
    positions = jnp.arange(seq_length)
    block_width = D // N_TP
    fringe_width = max(pool_windows) // 2
    for layer_idx in range(LAYERS):
        summed = jnp.zeros((seq_length, P_SIZE), jnp.float32)
        for block_idx in range(N_TP):
            first_col = block_idx * block_width
            partial_term = jnp.dot(stream[:, first_col:first_col + block_width], in_proj[layer_idx, first_col:first_col + block_width], preferred_element_type=jnp.float32).astype(jnp.bfloat16)
            summed = summed + partial_term.astype(jnp.float32)
        projected = summed.astype(jnp.bfloat16)
        proj_float = projected.astype(jnp.float32)
        padded = jnp.pad(proj_float, ((fringe_width, fringe_width), (0, 0)))
        mixed_parts = []
        for group_idx in range(4):
            span_len = pool_windows[group_idx]
            before = span_len // 2
            after = span_len - before
            group_cols = slice(group_idx * POOL_CH, (group_idx + 1) * POOL_CH)
            window_total = jnp.zeros((seq_length, POOL_CH), jnp.float32)
            for offset in range(-before, after):
                window_total = window_total + padded[fringe_width + offset:fringe_width + offset + seq_length, group_cols]
            low_edge = jnp.clip(positions - before, 0, seq_length)
            high_edge = jnp.clip(positions + after, 0, seq_length)
            pooled = window_total / (high_edge - low_edge).astype(jnp.float32)[:, None]
            differ = (pooled - proj_float[:, group_cols]).astype(jnp.bfloat16)
            mixed_parts.append(jnp.dot(differ, group_mix[layer_idx, group_idx], preferred_element_type=jnp.float32))
        mixed_out = (jnp.concatenate(mixed_parts, axis=1) * pool_gain[layer_idx][None, :]).astype(jnp.bfloat16)
        branch = jnp.dot(mixed_out, out_proj[layer_idx], preferred_element_type=jnp.float32)
        resid = residual_scale * stream.astype(jnp.float32) + branch
        row_mean = lax.optimization_barrier(jnp.mean(resid, axis=1, keepdims=True))
        row_var = lax.optimization_barrier(jnp.mean(jnp.square(resid - row_mean), axis=1, keepdims=True))
        normed = (resid - row_mean) * lax.rsqrt(row_var + norm_eps)
        stream = (normed * norm_gain[layer_idx][None, :] + norm_bias[layer_idx][None, :]).astype(jnp.bfloat16)
    return stream
```

```python
import functools

import jax
import jax.numpy as jnp
from jax import lax
from jax.experimental import pallas as pl
from jax.experimental.pallas import tpu as pltpu
from jax.sharding import Mesh
from jax.sharding import PartitionSpec as P

SP = ("z", "y")
norm_eps = 1e-05
REACH = 8
STAT = 16
F32, BF16 = jnp.float32, jnp.bfloat16


def nbytes(shapes):
    return sum(s.size * s.dtype.itemsize for s in shapes)


def kernel_call(body, out_shape, scratch=(), flops=0, in_specs=None, name=None, out_specs=None):
    def call(*args):
        specs = in_specs
        if specs is None:
            specs = [pl.BlockSpec(memory_space=pltpu.SMEM)]
            specs += [pl.BlockSpec(memory_space=pltpu.VMEM) for _ in args[1:]]
        outs = out_shape if isinstance(out_shape, (list, tuple)) else [out_shape]
        kw = {} if out_specs is None else {"out_specs": out_specs}
        return pl.pallas_call(
            body,
            out_shape=out_shape,
            in_specs=specs,
            scratch_shapes=list(scratch),
            cost_estimate=pl.CostEstimate(
                flops=flops, bytes_accessed=nbytes(args) + nbytes(outs), transcendentals=0
            ),
            name=name,
            **kw,
        )(*args)

    return call


def dot(a, b):
    return lax.dot_general(a, b, (((1,), (0,)), ((), ())), preferred_element_type=F32)


def dot_t(a, b):
    return lax.dot_general(a, b, (((1,), (1,)), ((), ())), preferred_element_type=F32)


def parts(v):
    hi = v.astype(BF16).astype(F32)
    mid = (v - hi).astype(BF16).astype(F32)
    low = (v - hi - mid).astype(BF16).astype(F32)
    return hi, mid, low


def project_body(sc, own, oth, w_own, w_oth, *outs):
    n = len(outs)
    width = outs[0].shape[1]
    for k in range(n):
        rows = pl.ds(((sc[0] + k) % n) * width, width)
        acc = dot_t(own[...], w_own[rows, :]) + dot_t(oth[...], w_oth[rows, :])
        outs[k][...] = acc.astype(BF16)


def pooled_mix(sc, proj, group_map, gain, out, seq_length):
    rows_in, rows_out = proj.shape[0], out.shape[0]
    half = lax.shift_left(jnp.int32(1), sc[0])
    base = sc[1]
    row = lax.broadcasted_iota(jnp.int32, (rows_out, rows_in), 0)
    col = lax.broadcasted_iota(jnp.int32, (rows_out, rows_in), 1) - REACH
    token = base + col
    inside = (col >= row - half) & (col < row + half) & (token >= 0) & (token < seq_length)
    band = jnp.where(inside, 1.0, 0.0).astype(BF16)
    at = base + lax.broadcasted_iota(jnp.int32, (rows_out, 1), 0)
    count = jnp.minimum(at + half, seq_length) - jnp.maximum(at - half, 0)
    count = jnp.maximum(count, 1).astype(F32)
    centre = proj.astype(F32)[REACH : REACH + rows_out]
    differ = (dot(band, proj) / count - centre).astype(BF16)
    out[...] = (dot(differ, group_map[...]) * gain[...]).astype(BF16)


def mix_first_body(sc, *refs, seq_length):
    *partials, group_map, gain, out = refs
    total = partials[0][...].astype(F32)
    for p in partials[1:]:
        total = total + p[...].astype(F32)
    pooled_mix(sc, total.astype(BF16), group_map, gain, out, seq_length)


def combine_stats(means, seconds, width):
    n = len(means)
    mean = means[0]
    for m in means[1:]:
        mean = mean + m
    mean = mean / n
    second = seconds[0] + width * jnp.square(means[0] - mean)
    for m, s in zip(means[1:], seconds[1:]):
        second = second + s + width * jnp.square(m - mean)
    return mean, lax.rsqrt(second / (n * width) + norm_eps)


def mix_body(sc, *refs, seq_length, width):
    *partials, group_map, gain, out, row_out = refs
    n = len(partials)
    rows = partials[0].shape[0] - 2 * STAT
    means, seconds, gw = [], [], []
    total, bw = None, None
    for p in partials:
        stat = jnp.concatenate(
            [p[rows : rows + STAT, :].astype(F32), p[rows + STAT :, :].astype(F32)], axis=1
        )
        means.append(stat[0:1] + stat[1:2] + stat[2:3])
        seconds.append(stat[3:4] + stat[4:5] + stat[5:6])
        chan = p[rows + STAT :, :].astype(F32)
        gw.append(chan[6:7] + chan[7:8] + chan[8:9])
        b = chan[9:10] + chan[10:11] + chan[11:12]
        bw = b if bw is None else bw + b
        q = p[0:rows, :].astype(F32)
        total = q if total is None else total + q
    mean, rstd = combine_stats(means, seconds, width)
    table = jnp.concatenate(
        [m - mean for m in means] + [mean, rstd, jnp.zeros((126 - n, mean.shape[1]), F32)], axis=0
    )
    table = jnp.transpose(table)[0:rows]
    row_out[...] = table
    for k in range(n):
        total = total + table[:, k : k + 1] * gw[k]
    proj = (total * table[:, n + 1 : n + 2] + bw).astype(BF16)
    pooled_mix(sc, proj, group_map, gain, out, seq_length)


def normed(resid, table, gain, bias, n):
    return (resid - table[:, n : n + 1]) * table[:, n + 1 : n + 2] * gain + bias


def branch_resid(sc, mixed, own, oth, o_own, o_oth, scale):
    n = len(mixed)
    width = mixed[0].shape[1]
    acc_own, acc_oth = scale * own, scale * oth
    for k in range(n):
        rows = pl.ds(((sc[0] + n - k) % n) * width, width)
        block = mixed[k][...]
        acc_own = acc_own + dot(block, o_own[rows, :])
        acc_oth = acc_oth + dot(block, o_oth[rows, :])
    return acc_own, acc_oth


def centred(own, oth):
    width = own.shape[1] + oth.shape[1]
    mean = (jnp.sum(own, 1, keepdims=True) + jnp.sum(oth, 1, keepdims=True)) / width
    own, oth = own - mean, oth - mean
    second = jnp.sum(own * own, 1, keepdims=True) + jnp.sum(oth * oth, 1, keepdims=True)
    return own, oth, mean, second


def stat_rows(columns, rows, lanes):
    place = lax.broadcasted_iota(jnp.int32, (rows, 128), 1)
    table = jnp.zeros((rows, 128), F32)
    for i, c in enumerate(columns):
        table = jnp.where(place == i, c, table)
    if lanes > rows:
        table = jnp.concatenate([table, jnp.zeros((lanes - rows, 128), F32)], axis=0)
    return jnp.transpose(table)[0:STAT]


def streams_in(refs, first, rows, n):
    if first:
        own, oth, *rest = refs
        keep = slice(REACH, REACH + rows)
        return own[...].astype(F32)[keep], oth[...].astype(F32)[keep], rest
    own, oth, table, g_own, b_own, g_oth, b_oth, *rest = refs
    keep = slice(REACH, REACH + rows)
    t = table[keep, :]
    s_own = normed(own[keep, :], t, g_own[...], b_own[...], n).astype(BF16).astype(F32)
    s_oth = normed(oth[keep, :], t, g_oth[...], b_oth[...], n).astype(BF16).astype(F32)
    return s_own, s_oth, rest


def layer_body(sc, *refs, n, first, scale):
    mixed, refs = refs[:n], refs[n:]
    rows = mixed[0].shape[0]
    own, oth, refs = streams_in(refs, first, rows, n)
    o_own, o_oth, w_own, w_oth, g_own, b_own, g_oth, b_oth, *refs = refs
    outs, (r_own, r_oth, lhs_own, lhs_oth) = refs[:n], refs[n:]
    own, oth = branch_resid(sc, mixed, own, oth, o_own, o_oth, scale)
    r_own[...] = own
    r_oth[...] = oth
    own, oth, mean, second = centred(own, oth)
    width = outs[0].shape[1]
    stats = stat_rows(parts(mean) + parts(second), rows, 2 * width)
    for lhs, value, gain, bias in ((lhs_own, own, g_own, b_own), (lhs_oth, oth, g_oth, b_oth)):
        lhs[0:rows, :] = (value * gain[...]).astype(BF16)
        extra = parts(gain[...]) + parts(bias[...])
        extra = jnp.concatenate(
            list(extra) + [jnp.zeros((STAT - 6, value.shape[1]), F32)], axis=0
        )
        lhs[rows : rows + STAT, :] = extra.astype(BF16)
    place = lax.broadcasted_iota(jnp.int32, (STAT, width), 0)
    for k in range(n):
        at = pl.ds(((sc[0] + k) % n) * width, width)
        acc = dot_t(lhs_own[...], w_own[at, :]) + dot_t(lhs_oth[...], w_oth[at, :])
        outs[k][0:rows, :] = acc[0:rows].astype(BF16)
        tail = acc[rows : rows + STAT]
        sums = parts(tail[0:1] + tail[1:2] + tail[2:3]) + parts(tail[3:4] + tail[4:5] + tail[5:6])
        block = stats[:, width:]
        for i, s in enumerate(sums):
            block = jnp.where(place == 6 + i, s, block)
        outs[k][rows : rows + STAT, :] = stats[:, :width].astype(BF16)
        outs[k][rows + STAT :, :] = block.astype(BF16)


def last_body(sc, *refs, n, first, scale):
    mixed, refs = refs[:n], refs[n:]
    rows = mixed[0].shape[0]
    own, oth, refs = streams_in(refs, first, rows, n)
    o_own, o_oth, r_own, r_oth, stats = refs
    own, oth = branch_resid(sc, mixed, own, oth, o_own, o_oth, scale)
    r_own[...] = own
    r_oth[...] = oth
    _, _, mean, second = centred(own, oth)
    stats[...] = stat_rows((mean, second), rows, stats.shape[1])[0:8]


def finish_body(sc, *refs, n, width):
    stats, refs = refs[:n], refs[n:]
    r_own, r_oth, g_own, b_own, g_oth, b_oth, out_own, out_oth = refs
    rows = r_own.shape[0]
    mean, rstd = combine_stats([s[0:1, :] for s in stats], [s[1:2, :] for s in stats], width)
    table = jnp.concatenate([mean, rstd, jnp.zeros((126, mean.shape[1]), F32)], axis=0)
    table = jnp.transpose(table)[0:rows]
    out_own[...] = normed(r_own[...], table, g_own[...], b_own[...], 0).astype(BF16)
    out_oth[...] = normed(r_oth[...], table, g_oth[...], b_oth[...], 0).astype(BF16)


def place_body(sc, *refs):
    *blocks, out, sems = refs
    n = len(blocks)
    copies = []
    for k, block in enumerate(blocks):
        at = (sc[2] + n - k) % n
        copies.append(pltpu.make_async_copy(block, out.at[:, :, at], sems.at[k]))
    for c in copies:
        c.start()
    for c in copies:
        c.wait()


def shifted(array, axis, step):
    n = lax.axis_size(axis)
    return lax.ppermute(array, axis, [(i, (i + step) % n) for i in range(n)])


def gathered(shard, sc):
    nz, ny = lax.axis_size("z"), lax.axis_size("y")
    spread = jnp.broadcast_to(shard[None], (nz, *shard.shape))
    over_z = lax.all_to_all(spread, "z", 0, 0, tiled=True)
    over_y = [over_z] + [shifted(over_z, "y", k) for k in range(1, ny)]
    out = jax.ShapeDtypeStruct((nz, shard.shape[0], ny, *shard.shape[1:]), shard.dtype)
    anywhere = pl.BlockSpec(memory_space=pl.ANY)
    placed = kernel_call(
        place_body,
        out,
        scratch=[pltpu.SemaphoreType.DMA((ny,))],
        in_specs=[pl.BlockSpec(memory_space=pltpu.SMEM)] + [anywhere] * ny,
        out_specs=anywhere,
        name="place",
    )(sc, *over_y)
    return placed


def on_device(tokens, in_proj, group_mix, pool_gain, out_proj, norm_gain, norm_bias):
    rows_dev, feat = tokens.shape
    layers = in_proj.shape[0]
    n = lax.axis_size("x")
    sp = lax.axis_size(SP)
    seq_length = rows_dev * sp
    channels = in_proj.shape[2] * sp
    group = channels // n
    half_rows = rows_dev // 2
    pad = layers * REACH
    scale = (2.0 * layers) ** 0.25
    x, c = lax.axis_index("x"), lax.axis_index("c")
    start = lax.axis_index(SP) * rows_dev + c * half_rows

    def scalars(base):
        return jnp.stack([x, base, lax.axis_index("y"), c]).astype(jnp.int32)

    sc = scalars(start)
    in_t = jnp.swapaxes(in_proj, 1, 2)

    def other(array):
        return lax.ppermute(array, "c", [(0, 1), (1, 0)])

    def weights(*shards):
        placed = gathered(jnp.stack(shards), sc)
        both = (placed, other(placed))

        def pick(i):
            return [b[:, i].reshape(channels, feat) for b in both]

        return [pick(i) for i in range(len(shards))]

    (w_in,) = weights(in_t[0])

    up = [(i, i + 1) for i in range(sp - 1)]
    before = lax.ppermute(tokens[rows_dev - pad :], SP, up)
    after = lax.ppermute(tokens[:pad], SP, [(j, i) for i, j in up])
    wide = jnp.concatenate([before, tokens, after], axis=0)
    length = half_rows + 2 * pad
    mine = lax.dynamic_slice_in_dim(wide, c * half_rows, length, 0)
    theirs = other(lax.dynamic_slice_in_dim(wide, (1 - c) * half_rows, length, 0))
    norm = jnp.concatenate([norm_gain, norm_bias], axis=0)
    norms = (norm, other(norm))
    maps = lax.dynamic_index_in_dim(group_mix, x, 1, keepdims=False)
    gains = lax.dynamic_slice_in_dim(pool_gain, x * group, group, 1)

    def norm_rows(l):
        return [a[i : i + 1] for a in norms for i in (l, layers + l)]

    def block(rows, width, dtype=BF16):
        return jax.ShapeDtypeStruct((rows, width), dtype)

    def exchanged(blocks):
        return [blocks[0]] + [shifted(b, "x", k) for k, b in enumerate(blocks) if k]

    rows = length
    flops = 2 * rows * 2 * feat * channels
    partials = kernel_call(
        project_body, [block(rows, group)] * n, flops=flops, name="project"
    )(sc, mine, theirs, *w_in)
    stream = [mine, theirs]
    w_next = [weights(out_proj[l], in_t[l + 1]) for l in range(layers - 1)]
    w_next.append(weights(out_proj[layers - 1]))
    for l in range(layers):
        first, last = l == 0, l == layers - 1
        arrived = exchanged(partials)
        done = rows - 2 * REACH
        here = scalars(start - pad + (l + 1) * REACH)
        mix_flops = 2 * done * group * (rows + group)
        if first:
            mixed = kernel_call(
                functools.partial(mix_first_body, seq_length=seq_length),
                block(done, group),
                flops=mix_flops,
                name="mix",
            )(here, *arrived, maps[l], gains[l : l + 1])
        else:
            mixed, table = kernel_call(
                functools.partial(mix_body, seq_length=seq_length, width=2 * feat),
                [block(done, group), block(rows, 128, F32)],
                flops=mix_flops,
                name="mix",
            )(here, *arrived, maps[l], gains[l : l + 1])
            stream = stream + [table] + norm_rows(l - 1)
        all_mixed = exchanged([mixed] * n)
        rows = done
        resid = [block(rows, feat, F32)] * 2
        if not last:
            (o_own, o_oth), (w_own, w_oth) = w_next[l]
            *partials, r_own, r_oth = kernel_call(
                functools.partial(layer_body, n=n, first=first, scale=scale),
                [block(rows + 2 * STAT, group)] * n + resid,
                scratch=[pltpu.VMEM((rows + STAT, feat), BF16)] * 2,
                flops=4 * rows * 2 * feat * channels,
                name="layer",
            )(here, *all_mixed, *stream, o_own, o_oth, w_own, w_oth, *norm_rows(l))
            stream = [r_own, r_oth]
        else:
            ((o_own, o_oth),) = w_next[l]
            r_own, r_oth, stats = kernel_call(
                functools.partial(last_body, n=n, first=first, scale=scale),
                resid + [block(8, rows, F32)],
                flops=2 * rows * 2 * feat * channels,
                name="last",
            )(here, *all_mixed, *stream, o_own, o_oth)
            out_own, out_oth = kernel_call(
                functools.partial(finish_body, n=n, width=2 * feat),
                [block(rows, feat)] * 2,
                name="finish",
            )(here, *exchanged([stats] * n), r_own, r_oth, *norm_rows(l))
    swapped = other(out_oth)
    return jnp.where(
        c == 0,
        jnp.concatenate([out_own, swapped], axis=0),
        jnp.concatenate([swapped, out_own], axis=0),
    )


def solution(mesh):
    split = Mesh(mesh.devices.reshape(8, 4, 4, 2), ("z", "y", "x", "c"))
    tp = ("x", "c")
    in_specs = (P(SP, tp), P(None, tp, SP), P(), P(), P(None, SP, tp), P(None, tp), P(None, tp))
    return jax.shard_map(
        on_device, mesh=split, in_specs=in_specs, out_specs=P(SP, tp), check_vma=False
    )
```

```python
import functools

import jax
import jax.numpy as jnp
from jax import lax
from jax.experimental import pallas as pl
from jax.experimental.pallas import tpu as pltpu
from jax.sharding import Mesh
from jax.sharding import PartitionSpec as P

SP = ("z", "y")
norm_eps = 1e-05
REACH = 8
STAT = 16
F32, BF16 = jnp.float32, jnp.bfloat16
VMEM_LIMIT = 20 * 2**20


def nbytes(shapes):
    return sum(s.size * s.dtype.itemsize for s in shapes)


def kernel_call(body, out_shape, scratch=(), flops=0, name=None, limit=VMEM_LIMIT):
    def call(*args):
        outs = out_shape if isinstance(out_shape, (list, tuple)) else [out_shape]
        specs = [pl.BlockSpec(memory_space=pltpu.SMEM)]
        specs += [pl.BlockSpec(memory_space=pltpu.VMEM) for _ in args[1:]]
        return pl.pallas_call(
            body,
            out_shape=out_shape,
            in_specs=specs,
            scratch_shapes=list(scratch),
            compiler_params=pltpu.CompilerParams(vmem_limit_bytes=limit),
            cost_estimate=pl.CostEstimate(
                flops=flops, bytes_accessed=nbytes(args) + nbytes(outs), transcendentals=0
            ),
            name=name,
        )(*args)

    return call


def dot(a, b):
    return lax.dot_general(a, b, (((1,), (0,)), ((), ())), preferred_element_type=F32)


def dot_t(a, b):
    return lax.dot_general(a, b, (((1,), (1,)), ((), ())), preferred_element_type=F32)


def parts(v):
    hi = v.astype(BF16).astype(F32)
    mid = (v - hi).astype(BF16).astype(F32)
    low = (v - hi - mid).astype(BF16).astype(F32)
    return hi, mid, low


def group_rows(blocks, g, n):
    per = blocks[0].shape[0] // n
    return jnp.concatenate([b[g * per + z] for z in range(per) for b in blocks], axis=0)


def take(refs, *counts):
    out = []
    for m in counts:
        out.append(refs[:m])
        refs = refs[m:]
    return *out, refs


def project_body(sc, own, oth, *refs, n, ny):
    w_own, w_oth, outs = take(refs, ny, ny)
    for k in range(n):
        g = (sc[0] + k) % n
        acc = dot_t(own[...], group_rows(w_own, g, n)) + dot_t(oth[...], group_rows(w_oth, g, n))
        outs[k][...] = acc.astype(BF16)


def pooled_mix(sc, proj, group_map, gain, out, seq_length, ny, piece):
    rows_in, rows_out = proj.shape[0], out.shape[0]
    half = lax.shift_left(jnp.int32(1), sc[0])
    base = sc[1]
    row = lax.broadcasted_iota(jnp.int32, (rows_out, rows_in), 0)
    col = lax.broadcasted_iota(jnp.int32, (rows_out, rows_in), 1) - REACH
    token = base + col
    inside = (col >= row - half) & (col < row + half) & (token >= 0) & (token < seq_length)
    band = jnp.where(inside, 1.0, 0.0).astype(BF16)
    at = base + lax.broadcasted_iota(jnp.int32, (rows_out, 1), 0)
    count = jnp.minimum(at + half, seq_length) - jnp.maximum(at - half, 0)
    count = jnp.maximum(count, 1).astype(F32)
    centre = proj.astype(F32)[REACH : REACH + rows_out]
    differ = (dot(band, proj) / count - centre).astype(BF16)
    width = proj.shape[1]
    true = lax.broadcasted_iota(jnp.int32, (width, width), 0)
    held = lax.broadcasted_iota(jnp.int32, (width, width), 1)
    z, k, i = held // (ny * piece), (held // piece) % ny, held % piece
    turn = jnp.where(true == (z * ny + (sc[2] + ny - k) % ny) * piece + i, 1.0, 0.0).astype(BF16)
    differ = dot_t(differ, turn).astype(BF16)
    mixed = (dot(differ, group_map[...]) * gain[...]).astype(BF16)
    out[...] = dot(mixed, turn).astype(BF16)


def mix_first_body(sc, *refs, **sizes):
    *partials, group_map, gain, out = refs
    total = partials[0][...].astype(F32)
    for p in partials[1:]:
        total = total + p[...].astype(F32)
    pooled_mix(sc, total.astype(BF16), group_map, gain, out, **sizes)


def combine_stats(means, seconds, width):
    n = len(means)
    mean = means[0]
    for m in means[1:]:
        mean = mean + m
    mean = mean / n
    second = seconds[0] + width * jnp.square(means[0] - mean)
    for m, s in zip(means[1:], seconds[1:]):
        second = second + s + width * jnp.square(m - mean)
    return mean, lax.rsqrt(second / (n * width) + norm_eps)


def mix_body(sc, *refs, width, **sizes):
    *partials, group_map, gain, out, row_out = refs
    n = len(partials)
    rows = partials[0].shape[0] - 2 * STAT
    means, seconds, gw = [], [], []
    total, bw = None, None
    for p in partials:
        stat = jnp.concatenate(
            [p[rows : rows + STAT, :].astype(F32), p[rows + STAT :, :].astype(F32)], axis=1
        )
        means.append(stat[0:1] + stat[1:2] + stat[2:3])
        seconds.append(stat[3:4] + stat[4:5] + stat[5:6])
        chan = p[rows + STAT :, :].astype(F32)
        gw.append(chan[6:7] + chan[7:8] + chan[8:9])
        b = chan[9:10] + chan[10:11] + chan[11:12]
        bw = b if bw is None else bw + b
        q = p[0:rows, :].astype(F32)
        total = q if total is None else total + q
    mean, rstd = combine_stats(means, seconds, width)
    table = jnp.concatenate(
        [m - mean for m in means] + [mean, rstd, jnp.zeros((126 - n, mean.shape[1]), F32)], axis=0
    )
    table = jnp.transpose(table)[0:rows]
    row_out[...] = table
    for k in range(n):
        total = total + table[:, k : k + 1] * gw[k]
    proj = (total * table[:, n + 1 : n + 2] + bw).astype(BF16)
    pooled_mix(sc, proj, group_map, gain, out, **sizes)


def normed(resid, table, gain, bias, n):
    return (resid - table[:, n : n + 1]) * table[:, n + 1 : n + 2] * gain + bias


def branch_resid(sc, mixed, own, oth, o_own, o_oth, scale):
    n = len(mixed)
    acc_own, acc_oth = scale * own, scale * oth
    for k in range(n):
        g = (sc[0] + n - k) % n
        block = mixed[k][...]
        acc_own = acc_own + dot(block, group_rows(o_own, g, n))
        acc_oth = acc_oth + dot(block, group_rows(o_oth, g, n))
    return acc_own, acc_oth


def centred(own, oth):
    width = own.shape[1] + oth.shape[1]
    mean = (jnp.sum(own, 1, keepdims=True) + jnp.sum(oth, 1, keepdims=True)) / width
    own, oth = own - mean, oth - mean
    second = jnp.sum(own * own, 1, keepdims=True) + jnp.sum(oth * oth, 1, keepdims=True)
    return own, oth, mean, second


def stat_rows(columns, rows, lanes):
    place = lax.broadcasted_iota(jnp.int32, (rows, 128), 1)
    table = jnp.zeros((rows, 128), F32)
    for i, c in enumerate(columns):
        table = jnp.where(place == i, c, table)
    if lanes > rows:
        table = jnp.concatenate([table, jnp.zeros((lanes - rows, 128), F32)], axis=0)
    return jnp.transpose(table)[0:STAT]


def streams_in(refs, first, rows, n):
    if first:
        own, oth, *rest = refs
        keep = slice(REACH, REACH + rows)
        return own[...].astype(F32)[keep], oth[...].astype(F32)[keep], rest
    own, oth, table, g_own, b_own, g_oth, b_oth, *rest = refs
    keep = slice(REACH, REACH + rows)
    t = table[keep, :]
    s_own = normed(own[keep, :], t, g_own[...], b_own[...], n).astype(BF16).astype(F32)
    s_oth = normed(oth[keep, :], t, g_oth[...], b_oth[...], n).astype(BF16).astype(F32)
    return s_own, s_oth, rest


def layer_body(sc, *refs, n, ny, first, scale):
    mixed, refs = refs[:n], refs[n:]
    rows = mixed[0].shape[0]
    own, oth, refs = streams_in(refs, first, rows, n)
    o_own, o_oth, w_own, w_oth, (g_own, b_own, g_oth, b_oth), refs = take(refs, ny, ny, ny, ny, 4)
    outs, (r_own, r_oth, lhs_own, lhs_oth) = refs[:n], refs[n:]
    own, oth = branch_resid(sc, mixed, own, oth, o_own, o_oth, scale)
    r_own[...] = own
    r_oth[...] = oth
    own, oth, mean, second = centred(own, oth)
    width = outs[0].shape[1]
    stats = stat_rows(parts(mean) + parts(second), rows, 2 * width)
    for lhs, value, gain, bias in ((lhs_own, own, g_own, b_own), (lhs_oth, oth, g_oth, b_oth)):
        lhs[0:rows, :] = (value * gain[...]).astype(BF16)
        extra = parts(gain[...]) + parts(bias[...])
        extra = jnp.concatenate(
            list(extra) + [jnp.zeros((STAT - 6, value.shape[1]), F32)], axis=0
        )
        lhs[rows : rows + STAT, :] = extra.astype(BF16)
    place = lax.broadcasted_iota(jnp.int32, (STAT, width), 0)
    for k in range(n):
        g = (sc[0] + k) % n
        acc = dot_t(lhs_own[...], group_rows(w_own, g, n))
        acc = acc + dot_t(lhs_oth[...], group_rows(w_oth, g, n))
        outs[k][0:rows, :] = acc[0:rows].astype(BF16)
        tail = acc[rows : rows + STAT]
        sums = parts(tail[0:1] + tail[1:2] + tail[2:3]) + parts(tail[3:4] + tail[4:5] + tail[5:6])
        block = stats[:, width:]
        for i, s in enumerate(sums):
            block = jnp.where(place == 6 + i, s, block)
        outs[k][rows : rows + STAT, :] = stats[:, :width].astype(BF16)
        outs[k][rows + STAT :, :] = block.astype(BF16)


def last_body(sc, *refs, n, ny, first, scale):
    mixed, refs = refs[:n], refs[n:]
    rows = mixed[0].shape[0]
    own, oth, refs = streams_in(refs, first, rows, n)
    o_own, o_oth, (r_own, r_oth, stats) = take(refs, ny, ny)
    own, oth = branch_resid(sc, mixed, own, oth, o_own, o_oth, scale)
    r_own[...] = own
    r_oth[...] = oth
    _, _, mean, second = centred(own, oth)
    stats[...] = stat_rows((mean, second), rows, stats.shape[1])[0:8]


def finish_body(sc, *refs, n, width):
    stats, refs = refs[:n], refs[n:]
    r_own, r_oth, g_own, b_own, g_oth, b_oth, out_own, out_oth = refs
    rows = r_own.shape[0]
    mean, rstd = combine_stats([s[0:1, :] for s in stats], [s[1:2, :] for s in stats], width)
    table = jnp.concatenate([mean, rstd, jnp.zeros((126, mean.shape[1]), F32)], axis=0)
    table = jnp.transpose(table)[0:rows]
    at = pl.ds(pl.multiple_of(sc[3] * rows, 16), rows)
    out_own[at, :] = normed(r_own[...], table, g_own[...], b_own[...], 0).astype(BF16)
    out_oth[...] = normed(r_oth[...], table, g_oth[...], b_oth[...], 0).astype(BF16)


def shifted(array, axis, step):
    n = lax.axis_size(axis)
    return lax.ppermute(array, axis, [(i, (i + step) % n) for i in range(n)])


def other(array):
    return lax.ppermute(array, "c", [(0, 1), (1, 0)])


def after(value, *events):
    return lax.optimization_barrier((value, *events))[0]


def over_z(*shards):
    shard = jnp.stack(shards)
    spread = jnp.broadcast_to(shard[None], (lax.axis_size("z"), *shard.shape))
    got = lax.all_to_all(spread, "z", 0, 0, tiled=True)
    return [got[:, i] for i in range(len(shards))]


def over_y(block):
    own = [block] + [shifted(block, "y", k) for k in range(1, lax.axis_size("y"))]
    return own + [other(b) for b in own]


def on_device(tokens, in_proj, group_mix, pool_gain, out_proj, norm_gain, norm_bias):
    rows_dev, feat = tokens.shape
    layers = in_proj.shape[0]
    n = lax.axis_size("x")
    sp = lax.axis_size(SP)
    seq_length = rows_dev * sp
    channels = in_proj.shape[2] * sp
    group = channels // n
    half_rows = rows_dev // 2
    pad = layers * REACH
    scale = (2.0 * layers) ** 0.25
    x, c = lax.axis_index("x"), lax.axis_index("c")
    start = lax.axis_index(SP) * rows_dev + c * half_rows

    def scalars(base):
        return jnp.stack([x, base, lax.axis_index("y"), c]).astype(jnp.int32)

    sc = scalars(start)
    ny = lax.axis_size("y")
    sizes = dict(seq_length=seq_length, ny=ny, piece=in_proj.shape[2])
    in_t = jnp.swapaxes(in_proj, 1, 2)
    (z_in,) = over_z(in_t[0])
    w_in = over_y(z_in)

    up = [(i, i + 1) for i in range(sp - 1)]
    before = lax.ppermute(tokens[rows_dev - pad :], SP, up)
    behind = lax.ppermute(tokens[:pad], SP, [(j, i) for i, j in up])
    wide = jnp.concatenate([before, tokens, behind], axis=0)
    length = half_rows + 2 * pad
    mine = lax.dynamic_slice_in_dim(wide, c * half_rows, length, 0)
    theirs = other(lax.dynamic_slice_in_dim(wide, (1 - c) * half_rows, length, 0))
    norm = jnp.concatenate([norm_gain, norm_bias], axis=0)
    norms = (norm, other(norm))
    maps = lax.dynamic_index_in_dim(group_mix, x, 1, keepdims=False)
    gains = lax.dynamic_slice_in_dim(pool_gain, x * group, group, 1)

    def norm_rows(l):
        return [a[i : i + 1] for a in norms for i in (l, layers + l)]

    def block(rows, width, dtype=BF16):
        return jax.ShapeDtypeStruct((rows, width), dtype)

    def exchanged(blocks):
        return [blocks[0]] + [shifted(b, "x", k) for k, b in enumerate(blocks) if k]

    rows = length
    flops = 2 * rows * 2 * feat * channels
    partials = kernel_call(
        functools.partial(project_body, n=n, ny=ny),
        [block(rows, group)] * n,
        flops=flops,
        name="project",
    )(sc, mine, theirs, *w_in)
    stream = [mine, theirs]
    z_next = over_z(after(out_proj[0], z_in), in_t[1])
    for l in range(layers):
        first, last = l == 0, l == layers - 1
        arrived = exchanged(partials)
        o_w = over_y(after(z_next.pop(0), partials[0]))
        done = rows - 2 * REACH
        here = scalars(start - pad + (l + 1) * REACH)
        mix_flops = 2 * done * group * (rows + group)
        if first:
            mixed = kernel_call(
                functools.partial(mix_first_body, **sizes),
                block(done, group),
                flops=mix_flops,
                name="mix",
            )(here, *arrived, maps[l], gains[l : l + 1])
        else:
            mixed, table = kernel_call(
                functools.partial(mix_body, width=2 * feat, **sizes),
                [block(done, group), block(rows, 128, F32)],
                flops=mix_flops,
                name="mix",
            )(here, *arrived, maps[l], gains[l : l + 1])
            stream = stream + [table] + norm_rows(l - 1)
        all_mixed = exchanged([mixed] * n)
        if not last:
            w_w = over_y(after(z_next.pop(0), mixed))
        if first:
            todo = [w for i in range(1, layers) for w in (out_proj[i], in_t[i + 1 : i + 2])]
            todo = [w.reshape(w.shape[-2:]) for w in todo if w.size]
            z_next = over_z(after(todo[0], mixed), *todo[1:])
        rows = done
        resid = [block(rows, feat, F32)] * 2
        if not last:
            *partials, r_own, r_oth = kernel_call(
                functools.partial(layer_body, n=n, ny=ny, first=first, scale=scale),
                [block(rows + 2 * STAT, group)] * n + resid,
                scratch=[pltpu.VMEM((rows + STAT, feat), BF16)] * 2,
                flops=4 * rows * 2 * feat * channels,
                name="layer",
            )(here, *all_mixed, *stream, *o_w, *w_w, *norm_rows(l))
            stream = [r_own, r_oth]
        else:
            r_own, r_oth, stats = kernel_call(
                functools.partial(last_body, n=n, ny=ny, first=first, scale=scale),
                resid + [block(8, rows, F32)],
                flops=2 * rows * 2 * feat * channels,
                name="last",
            )(here, *all_mixed, *stream, *o_w)
            out_own, out_oth = kernel_call(
                functools.partial(finish_body, n=n, width=2 * feat),
                [block(rows_dev, feat), block(rows, feat)],
                name="finish",
            )(here, *exchanged([stats] * n), r_own, r_oth, *norm_rows(l))
    return lax.dynamic_update_slice_in_dim(out_own, other(out_oth), (1 - c) * half_rows, 0)


def solution(mesh):
    split = Mesh(mesh.devices.reshape(8, 4, 4, 2), ("z", "y", "x", "c"))
    tp = ("x", "c")
    in_specs = (P(SP, tp), P(None, tp, SP), P(), P(), P(None, SP, tp), P(None, tp), P(None, tp))
    return jax.shard_map(
        on_device, mesh=split, in_specs=in_specs, out_specs=P(SP, tp), check_vma=False
    )
```

```python
import functools

import jax
import jax.numpy as jnp
from jax import lax
from jax.experimental import pallas as pl
from jax.experimental.pallas import tpu as pltpu
from jax.sharding import Mesh
from jax.sharding import PartitionSpec as P


SP = ("z", "y")
norm_eps = 1e-05
REACH = 8
STAT = 16
F32, BF16 = jnp.float32, jnp.bfloat16
VMEM_LIMIT = 20 * 2**20


def nbytes(shapes):
    return sum(s.size * s.dtype.itemsize for s in shapes)


def kernel_call(body, out_shape, scratch=(), flops=0, limit=VMEM_LIMIT):
    def call(*args):
        outs = out_shape if isinstance(out_shape, (list, tuple)) else [out_shape]
        specs = [pl.BlockSpec(memory_space=pltpu.SMEM)]
        specs += [pl.BlockSpec(memory_space=pltpu.VMEM) for _ in args[1:]]
        return pl.pallas_call(
            body,
            out_shape=out_shape,
            in_specs=specs,
            scratch_shapes=list(scratch),
            compiler_params=pltpu.CompilerParams(vmem_limit_bytes=limit),
            cost_estimate=pl.CostEstimate(
                flops=flops, bytes_accessed=nbytes(args) + nbytes(outs), transcendentals=0
            ),
        )(*args)

    return call


def dot(a, b):
    return lax.dot_general(a, b, (((1,), (0,)), ((), ())), preferred_element_type=F32)


def dot_t(a, b):
    return lax.dot_general(a, b, (((1,), (1,)), ((), ())), preferred_element_type=F32)


def parts(v):
    hi = v.astype(BF16).astype(F32)
    mid = (v - hi).astype(BF16).astype(F32)
    low = (v - hi - mid).astype(BF16).astype(F32)
    return hi, mid, low


def group_rows(weights, m, g, n):
    stacked = len(weights) == 1
    count = weights[0].shape[0] if stacked else len(weights)
    ref = weights[0]
    per = ref.shape[1 if stacked else 0] // n
    rows = [
        ref[k, g * per + z, m] if stacked else weights[k][g * per + z, m]
        for z in range(per)
        for k in range(count)
    ]
    return jnp.concatenate(rows, axis=0)


def take(refs, *counts):
    out = []
    for m in counts:
        out.append(refs[:m])
        refs = refs[m:]
    return *out, refs


def project_body(sc, own, oth, *refs, n, held):
    w_own, w_oth, outs = take(refs, *held)
    for k in range(n):
        g = (sc[0] + k) % n
        acc = dot_t(own[...], group_rows(w_own, 0, g, n))
        acc = acc + dot_t(oth[...], group_rows(w_oth, 0, g, n))
        outs[k][...] = acc.astype(BF16)


def pooled_mix(sc, proj, group_map, gain, out, seq_length, ny, piece):
    rows_in, rows_out = proj.shape[0], out.shape[0]
    half = lax.shift_left(jnp.int32(1), sc[0])
    base = sc[1]
    row = lax.broadcasted_iota(jnp.int32, (rows_out, rows_in), 0)
    col = lax.broadcasted_iota(jnp.int32, (rows_out, rows_in), 1) - REACH
    token = base + col
    inside = (col >= row - half) & (col < row + half) & (token >= 0) & (token < seq_length)
    band = jnp.where(inside, 1.0, 0.0).astype(BF16)
    at = base + lax.broadcasted_iota(jnp.int32, (rows_out, 1), 0)
    count = jnp.minimum(at + half, seq_length) - jnp.maximum(at - half, 0)
    count = jnp.maximum(count, 1).astype(F32)
    centre = proj.astype(F32)[REACH : REACH + rows_out]
    differ = (dot(band, proj) / count - centre).astype(BF16)
    width = proj.shape[1]
    true = lax.broadcasted_iota(jnp.int32, (width, width), 0)
    held = lax.broadcasted_iota(jnp.int32, (width, width), 1)
    z, k, i = held // (ny * piece), (held // piece) % ny, held % piece
    turn = jnp.where(true == (z * ny + (sc[2] + ny - k) % ny) * piece + i, 1.0, 0.0).astype(BF16)
    differ = dot_t(differ, turn).astype(BF16)
    mixed = (dot(differ, group_map[...]) * gain[...]).astype(BF16)
    out[...] = dot(mixed, turn).astype(BF16)


def mix_first_body(sc, *refs, **sizes):
    *partials, group_map, gain, out = refs
    total = partials[0][...].astype(F32)
    for p in partials[1:]:
        total = total + p[...].astype(F32)
    pooled_mix(sc, total.astype(BF16), group_map, gain, out, **sizes)


def combine_stats(means, seconds, width):
    n = len(means)
    mean = means[0]
    for m in means[1:]:
        mean = mean + m
    mean = mean / n
    second = seconds[0] + width * jnp.square(means[0] - mean)
    for m, s in zip(means[1:], seconds[1:]):
        second = second + s + width * jnp.square(m - mean)
    return mean, lax.rsqrt(second / (n * width) + norm_eps)


def mix_body(sc, *refs, width, **sizes):
    *partials, group_map, gain, out, row_out = refs
    n = len(partials)
    rows = partials[0].shape[0] - 2 * STAT
    means, seconds, gw = [], [], []
    total, bw = None, None
    for p in partials:
        stat = jnp.concatenate(
            [p[rows : rows + STAT, :].astype(F32), p[rows + STAT :, :].astype(F32)], axis=1
        )
        means.append(stat[0:1] + stat[1:2] + stat[2:3])
        seconds.append(stat[3:4] + stat[4:5] + stat[5:6])
        chan = p[rows + STAT :, :].astype(F32)
        gw.append(chan[6:7] + chan[7:8] + chan[8:9])
        b = chan[9:10] + chan[10:11] + chan[11:12]
        bw = b if bw is None else bw + b
        q = p[0:rows, :].astype(F32)
        total = q if total is None else total + q
    mean, rstd = combine_stats(means, seconds, width)
    table = jnp.concatenate(
        [m - mean for m in means] + [mean, rstd, jnp.zeros((126 - n, mean.shape[1]), F32)], axis=0
    )
    table = jnp.transpose(table)[0:rows]
    row_out[...] = table
    for k in range(n):
        total = total + table[:, k : k + 1] * gw[k]
    proj = (total * table[:, n + 1 : n + 2] + bw).astype(BF16)
    pooled_mix(sc, proj, group_map, gain, out, **sizes)


def normed(resid, table, gain, bias, n):
    return (resid - table[:, n : n + 1]) * table[:, n + 1 : n + 2] * gain + bias


def branch_resid(sc, mixed, own, oth, w_own, w_oth, m, scale):
    n = len(mixed)
    acc_own, acc_oth = scale * own, scale * oth
    for k in range(n):
        g = (sc[0] + n - k) % n
        block = mixed[k][...]
        acc_own = acc_own + dot(block, group_rows(w_own, m, g, n))
        acc_oth = acc_oth + dot(block, group_rows(w_oth, m, g, n))
    return acc_own, acc_oth


def centred(own, oth):
    width = own.shape[1] + oth.shape[1]
    mean = (jnp.sum(own, 1, keepdims=True) + jnp.sum(oth, 1, keepdims=True)) / width
    own, oth = own - mean, oth - mean
    second = jnp.sum(own * own, 1, keepdims=True) + jnp.sum(oth * oth, 1, keepdims=True)
    return own, oth, mean, second


def stat_rows(columns, rows, lanes):
    place = lax.broadcasted_iota(jnp.int32, (rows, 128), 1)
    table = jnp.zeros((rows, 128), F32)
    for i, c in enumerate(columns):
        table = jnp.where(place == i, c, table)
    if lanes > rows:
        table = jnp.concatenate([table, jnp.zeros((lanes - rows, 128), F32)], axis=0)
    return jnp.transpose(table)[0:STAT]


def streams_in(refs, first, rows, n):
    if first:
        own, oth, *rest = refs
        keep = slice(REACH, REACH + rows)
        return own[...].astype(F32)[keep], oth[...].astype(F32)[keep], rest
    own, oth, table, g_own, b_own, g_oth, b_oth, *rest = refs
    keep = slice(REACH, REACH + rows)
    t = table[keep, :]
    s_own = normed(own[keep, :], t, g_own[...], b_own[...], n).astype(BF16).astype(F32)
    s_oth = normed(oth[keep, :], t, g_oth[...], b_oth[...], n).astype(BF16).astype(F32)
    return s_own, s_oth, rest


def layer_body(sc, *refs, n, held, first, scale):
    mixed, refs = refs[:n], refs[n:]
    rows = mixed[0].shape[0]
    own, oth, refs = streams_in(refs, first, rows, n)
    w_own, w_oth, (g_own, b_own, g_oth, b_oth), refs = take(refs, *held, 4)
    outs, (r_own, r_oth, lhs_own, lhs_oth) = refs[:n], refs[n:]
    own, oth = branch_resid(sc, mixed, own, oth, w_own, w_oth, 0, scale)
    r_own[...] = own
    r_oth[...] = oth
    own, oth, mean, second = centred(own, oth)
    width = outs[0].shape[1]
    stats = stat_rows(parts(mean) + parts(second), rows, 2 * width)
    for lhs, value, gain, bias in ((lhs_own, own, g_own, b_own), (lhs_oth, oth, g_oth, b_oth)):
        lhs[0:rows, :] = (value * gain[...]).astype(BF16)
        extra = parts(gain[...]) + parts(bias[...])
        extra = jnp.concatenate(
            list(extra) + [jnp.zeros((STAT - 6, value.shape[1]), F32)], axis=0
        )
        lhs[rows : rows + STAT, :] = extra.astype(BF16)
    place = lax.broadcasted_iota(jnp.int32, (STAT, width), 0)
    for k in range(n):
        g = (sc[0] + k) % n
        acc = dot_t(lhs_own[...], group_rows(w_own, 1, g, n))
        acc = acc + dot_t(lhs_oth[...], group_rows(w_oth, 1, g, n))
        outs[k][0:rows, :] = acc[0:rows].astype(BF16)
        tail = acc[rows : rows + STAT]
        sums = parts(tail[0:1] + tail[1:2] + tail[2:3]) + parts(tail[3:4] + tail[4:5] + tail[5:6])
        block = stats[:, width:]
        for i, s in enumerate(sums):
            block = jnp.where(place == 6 + i, s, block)
        outs[k][rows : rows + STAT, :] = stats[:, :width].astype(BF16)
        outs[k][rows + STAT :, :] = block.astype(BF16)


def last_body(sc, *refs, n, held, first, scale):
    mixed, refs = refs[:n], refs[n:]
    rows = mixed[0].shape[0]
    own, oth, refs = streams_in(refs, first, rows, n)
    w_own, w_oth, (r_own, r_oth, stats) = take(refs, *held)
    own, oth = branch_resid(sc, mixed, own, oth, w_own, w_oth, 0, scale)
    r_own[...] = own
    r_oth[...] = oth
    _, _, mean, second = centred(own, oth)
    stats[...] = stat_rows((mean, second), rows, stats.shape[1])[0:8]


def finish_body(sc, *refs, n, width):
    stats, refs = refs[:n], refs[n:]
    r_own, r_oth, g_own, b_own, g_oth, b_oth, out_own, out_oth = refs
    rows = r_own.shape[0]
    mean, rstd = combine_stats([s[0:1, :] for s in stats], [s[1:2, :] for s in stats], width)
    table = jnp.concatenate([mean, rstd, jnp.zeros((126, mean.shape[1]), F32)], axis=0)
    table = jnp.transpose(table)[0:rows]
    at = pl.ds(pl.multiple_of(sc[3] * rows, 16), rows)
    out_own[at, :] = normed(r_own[...], table, g_own[...], b_own[...], 0).astype(BF16)
    out_oth[...] = normed(r_oth[...], table, g_oth[...], b_oth[...], 0).astype(BF16)


def shifted(array, axis, step):
    n = lax.axis_size(axis)
    return lax.ppermute(array, axis, [(i, (i + step) % n) for i in range(n)])


def other(array):
    return lax.ppermute(array, "c", [(0, 1), (1, 0)])


def after(value, *events):
    return lax.optimization_barrier((value, *events))[0]


def over_z(shards):
    spread = jnp.broadcast_to(shards[None], (lax.axis_size("z"), *shards.shape))
    return lax.all_to_all(spread, "z", 0, 0, tiled=True)


def over_y(block):
    return [block] + [shifted(block, "y", k) for k in range(1, lax.axis_size("y"))]


def over_c(own, stacked):
    if stacked:
        own = [jnp.stack(own)]
    return own, [other(b) for b in own]


def layers_on_device(tokens, in_proj, group_mix, pool_gain, out_proj, norm_gain, norm_bias):
    rows_dev, feat = tokens.shape
    layers = in_proj.shape[0]
    n = lax.axis_size("x")
    sp = lax.axis_size(SP)
    seq_length = rows_dev * sp
    channels = in_proj.shape[2] * sp
    group = channels // n
    half_rows = rows_dev // 2
    pad = layers * REACH
    scale = (2.0 * layers) ** 0.25
    x, c = lax.axis_index("x"), lax.axis_index("c")
    start = lax.axis_index(SP) * rows_dev + c * half_rows

    def scalars(base):
        return jnp.stack([x, base, lax.axis_index("y"), c]).astype(jnp.int32)

    sc = scalars(start)
    ny = lax.axis_size("y")
    sizes = dict(seq_length=seq_length, ny=ny, piece=in_proj.shape[2])
    z_in = over_z(jnp.swapaxes(in_proj[:1], 1, 2))
    w_in = over_c(over_y(z_in), False)
    in_rest = jnp.swapaxes(after(in_proj[1:], z_in), 1, 2)

    up = [(i, i + 1) for i in range(sp - 1)]
    before = lax.ppermute(tokens[rows_dev - pad :], SP, up)
    behind = lax.ppermute(tokens[:pad], SP, [(j, i) for i, j in up])
    wide = jnp.concatenate([before, tokens, behind], axis=0)
    length = half_rows + 2 * pad
    mine = lax.dynamic_slice_in_dim(wide, c * half_rows, length, 0)
    theirs = other(lax.dynamic_slice_in_dim(wide, (1 - c) * half_rows, length, 0))
    norm = jnp.concatenate([norm_gain, norm_bias], axis=0)
    norms = (norm, other(norm))
    maps = lax.dynamic_index_in_dim(group_mix, x, 1, keepdims=False)
    gains = lax.dynamic_slice_in_dim(pool_gain, x * group, group, 1)

    def norm_rows(l):
        return [a[i : i + 1] for a in norms for i in (l, layers + l)]

    def block(rows, width, dtype=BF16):
        return jax.ShapeDtypeStruct((rows, width), dtype)

    def exchanged(blocks):
        return [blocks[0]] + [shifted(b, "x", k) for k, b in enumerate(blocks) if k]

    rows = length
    flops = 2 * rows * 2 * feat * channels
    partials = kernel_call(
        functools.partial(project_body, n=n, held=(len(w_in[0]), len(w_in[1]))),
        [block(rows, group)] * n,
        flops=flops,
    )(sc, mine, theirs, *w_in[0], *w_in[1])
    stream = [mine, theirs]
    pairs = [jnp.stack([out_proj[l], in_rest[l]]) for l in range(layers - 1)]
    pairs.append(out_proj[layers - 1 :])
    z_sets = [over_z(pairs[0])]
    for l in range(layers):
        first, last = l == 0, l == layers - 1
        arrived = exchanged(partials)
        y_w = over_y(after(z_sets[l], partials[0]))
        done = rows - 2 * REACH
        here = scalars(start - pad + (l + 1) * REACH)
        mix_flops = 2 * done * group * (rows + group)
        if first:
            mixed = kernel_call(
                functools.partial(mix_first_body, **sizes), block(done, group), flops=mix_flops
            )(here, *arrived, maps[l], gains[l : l + 1])
        else:
            mixed, table = kernel_call(
                functools.partial(mix_body, width=2 * feat, **sizes),
                [block(done, group), block(rows, 128, F32)],
                flops=mix_flops,
            )(here, *arrived, maps[l], gains[l : l + 1])
            stream = stream + [table] + norm_rows(l - 1)
        all_mixed = exchanged([mixed] * n)
        y_w = lax.optimization_barrier((*y_w, mixed))[:-1]
        own_w, oth_w = over_c(list(y_w), not first)
        held = (len(own_w), len(oth_w))
        if first:
            rest = over_z(after(jnp.concatenate(pairs[1:], axis=0), z_sets[0], partials[0]))
            z_sets += [rest[:, 2 * i : 2 * i + 2] for i in range(layers - 1)]
        rows = done
        resid = [block(rows, feat, F32)] * 2
        if not last:
            *partials, r_own, r_oth = kernel_call(
                functools.partial(layer_body, n=n, held=held, first=first, scale=scale),
                [block(rows + 2 * STAT, group)] * n + resid,
                scratch=[pltpu.VMEM((rows + STAT, feat), BF16)] * 2,
                flops=4 * rows * 2 * feat * channels,
            )(here, *all_mixed, *stream, *own_w, *oth_w, *norm_rows(l))
            stream = [r_own, r_oth]
        else:
            r_own, r_oth, stats = kernel_call(
                functools.partial(last_body, n=n, held=held, first=first, scale=scale),
                resid + [block(8, rows, F32)],
                flops=2 * rows * 2 * feat * channels,
            )(here, *all_mixed, *stream, *own_w, *oth_w)
            out_own, out_oth = kernel_call(
                functools.partial(finish_body, n=n, width=2 * feat),
                [block(rows_dev, feat), block(rows, feat)],
            )(here, *exchanged([stats] * n), r_own, r_oth, *norm_rows(l))
    return lax.dynamic_update_slice_in_dim(out_own, other(out_oth), (1 - c) * half_rows, 0)


def solution(mesh):
    split = Mesh(mesh.devices.reshape(8, 4, 4, 2), ("z", "y", "x", "c"))
    tp = ("x", "c")
    in_specs = (P(SP, tp), P(None, tp, SP), P(), P(), P(None, SP, tp), P(None, tp), P(None, tp))
    return jax.shard_map(
        layers_on_device, mesh=split, in_specs=in_specs, out_specs=P(SP, tp), check_vma=False
    )
```

```python
import functools

import jax
import jax.numpy as jnp
from jax import lax
from jax.experimental import pallas as pl
from jax.experimental.pallas import tpu as pltpu
from jax.sharding import Mesh
from jax.sharding import PartitionSpec as P


SP = ("z", "y")
norm_eps = 1e-05
REACH = 8
STAT = 16
F32, BF16 = jnp.float32, jnp.bfloat16
CORE_RUNS = (2, 2)
LIMITS = (60 * 2**20, 20 * 2**20)
VMEM_LIMIT = 20 * 2**20


def nbytes(shapes):
    return sum(s.size * s.dtype.itemsize for s in shapes)


def kernel_call(body, out_shape, scratch=(), flops=0, limit=VMEM_LIMIT, in_hbm=()):
    def call(*args):
        outs = out_shape if isinstance(out_shape, (list, tuple)) else [out_shape]
        specs = [pl.BlockSpec(memory_space=pltpu.SMEM)]
        specs += [
            pl.BlockSpec(memory_space=pl.ANY if i in in_hbm else pltpu.VMEM)
            for i in range(1, len(args))
        ]
        return pl.pallas_call(
            body,
            out_shape=out_shape,
            in_specs=specs,
            scratch_shapes=list(scratch),
            compiler_params=pltpu.CompilerParams(vmem_limit_bytes=limit),
            cost_estimate=pl.CostEstimate(
                flops=flops, bytes_accessed=nbytes(args) + nbytes(outs), transcendentals=0
            ),
        )(*args)

    return call


def dot(a, b):
    return lax.dot_general(a, b, (((1,), (0,)), ((), ())), preferred_element_type=F32)


def dot_t(a, b):
    return lax.dot_general(a, b, (((1,), (1,)), ((), ())), preferred_element_type=F32)


def parts(v):
    hi = v.astype(BF16).astype(F32)
    mid = (v - hi).astype(BF16).astype(F32)
    low = (v - hi - mid).astype(BF16).astype(F32)
    return hi, mid, low


def group_rows(weights, m, g, n):
    per = weights[0].shape[1] // n
    rows = [
        w[k, g * per + z, m] for z in range(per) for w in weights for k in range(w.shape[0])
    ]
    return jnp.concatenate(rows, axis=0)


def feature_rows(own, oth, m, g, n):
    return jnp.concatenate([group_rows(own, m, g, n), group_rows(oth, m, g, n)], axis=1)


def take(refs, *counts):
    out = []
    for m in counts:
        out.append(refs[:m])
        refs = refs[m:]
    return *out, refs


def project_body(sc, own, oth, *refs, n, held):
    w_own, w_oth, (*outs, held_out) = take(refs, *held)

    def project_group(k, carry):
        both = jnp.concatenate([own[...], oth[0 : own.shape[0], :]], axis=1)
        acc = dot_t(both, feature_rows(w_own, w_oth, 0, (sc[0] + k) % n, n))
        held_out[k] = acc.astype(BF16)
        return carry

    lax.fori_loop(0, n, project_group, 0)
    for k in range(n):
        outs[k][...] = held_out[k]


def pooled_mix(sc, proj, fetch, group_map, gains, out, layer, seq_length, ny, piece):
    rows_in, rows_out = proj.shape[0], out.shape[0]
    half = lax.shift_left(jnp.int32(1), sc[0])
    base = sc[1]
    col = lax.broadcasted_iota(jnp.int32, (rows_out, rows_in), 1) - REACH
    at = lax.broadcasted_iota(jnp.int32, (rows_out, 1), 0)
    low = jnp.maximum(at - half, -base)
    high = jnp.minimum(at + half, seq_length - base)
    band = jnp.where((col >= low) & (col < high), 1.0, 0.0).astype(BF16)
    count = jnp.maximum(high - low, 1).astype(F32)
    centre = proj.astype(F32)[REACH : REACH + rows_out]
    differ = (dot(band, proj) / count - centre).astype(BF16)
    width = proj.shape[1]
    true = lax.broadcasted_iota(jnp.int32, (width, width), 0)
    held = lax.broadcasted_iota(jnp.int32, (width, width), 1)
    z, k, i = held // (ny * piece), (held // piece) % ny, held % piece
    turn = jnp.where(true == (z * ny + (sc[2] + ny - k) % ny) * piece + i, 1.0, 0.0).astype(BF16)
    differ = dot_t(differ, turn).astype(BF16)
    gain = gains[layer : layer + 1, 0:width]
    for g in range(1, gains.shape[1] // width):
        gain = jnp.where(sc[0] == g, gains[layer : layer + 1, g * width : (g + 1) * width], gain)
    fetch.wait()
    mixed = (dot(differ, group_map[...]) * gain).astype(BF16)
    out[...] = dot(mixed, turn).astype(BF16)


def mix_first_body(sc, *refs, **sizes):
    *partials, maps, gains, out, group_map, sem = refs
    fetch = pltpu.make_async_copy(maps.at[sizes["layer"], sc[0]], group_map, sem)
    fetch.start()
    total = partials[0][...].astype(F32)
    for p in partials[1:]:
        total = total + p[...].astype(F32)
    pooled_mix(sc, total.astype(BF16), fetch, group_map, gains, out, **sizes)


def combine_stats(means, seconds, width):
    n = len(means)
    mean = means[0]
    for m in means[1:]:
        mean = mean + m
    mean = mean / n
    second = seconds[0] + width * jnp.square(means[0] - mean)
    for m, s in zip(means[1:], seconds[1:]):
        second = second + s + width * jnp.square(m - mean)
    return mean, lax.rsqrt(second / (n * width) + norm_eps)


def mix_body(sc, *refs, width, **sizes):
    *partials, maps, gains, out, row_out, group_map, sem = refs
    fetch = pltpu.make_async_copy(maps.at[sizes["layer"], sc[0]], group_map, sem)
    fetch.start()
    n = len(partials)
    rows = partials[0].shape[0] - 2 * STAT
    means, seconds, gw = [], [], []
    total, bw = None, None
    for p in partials:
        stat = jnp.concatenate(
            [p[rows : rows + STAT, :].astype(F32), p[rows + STAT :, :].astype(F32)], axis=1
        )
        means.append(stat[0:1] + stat[1:2] + stat[2:3])
        seconds.append(stat[3:4] + stat[4:5] + stat[5:6])
        chan = p[rows + STAT :, :].astype(F32)
        gw.append(chan[6:7] + chan[7:8] + chan[8:9])
        b = chan[9:10] + chan[10:11] + chan[11:12]
        bw = b if bw is None else bw + b
        q = p[0:rows, :].astype(F32)
        total = q if total is None else total + q
    mean, rstd = combine_stats(means, seconds, width)
    table = jnp.concatenate(
        [m - mean for m in means] + [mean, rstd, jnp.zeros((126 - n, mean.shape[1]), F32)], axis=0
    )
    table = jnp.transpose(table)[0:rows]
    row_out[...] = table
    for k in range(n):
        total = total + table[:, k : k + 1] * gw[k]
    proj = (total * table[:, n + 1 : n + 2] + bw).astype(BF16)
    pooled_mix(sc, proj, fetch, group_map, gains, out, **sizes)


def normed(resid, table, gain, bias, n):
    return (resid - table[:, n : n + 1]) * table[:, n + 1 : n + 2] * gain + bias


def branch_resid(sc, mixed, own, oth, w_own, w_oth, m, scale):
    n = len(mixed)
    block = jnp.concatenate([b[...] for b in mixed], axis=1)
    order = [(sc[0] + n - k) % n for k in range(n)]

    def branch(weights):
        return dot(block, jnp.concatenate([group_rows(weights, m, g, n) for g in order], axis=0))

    return scale * own + branch(w_own), scale * oth + branch(w_oth)


def centred(own, oth):
    width = own.shape[1] + oth.shape[1]
    mean = (jnp.sum(own, 1, keepdims=True) + jnp.sum(oth, 1, keepdims=True)) / width
    own, oth = own - mean, oth - mean
    second = jnp.sum(own * own, 1, keepdims=True) + jnp.sum(oth * oth, 1, keepdims=True)
    return own, oth, mean, second


def stat_rows(columns, rows, lanes):
    place = lax.broadcasted_iota(jnp.int32, (rows, 128), 1)
    table = jnp.zeros((rows, 128), F32)
    for i, c in enumerate(columns):
        table = jnp.where(place == i, c, table)
    if lanes > rows:
        table = jnp.concatenate([table, jnp.zeros((lanes - rows, 128), F32)], axis=0)
    return jnp.transpose(table)[0:STAT]


def norm_rows(norm, layer):
    layers = norm.shape[0] // 2
    return norm[layer : layer + 1, :], norm[layers + layer : layers + layer + 1, :]


def carried(slab, count):
    tail = slab[slab.shape[0] - 2 * STAT :, :].astype(F32)
    return tail[0:count] + tail[8 : 8 + count] + tail[16 : 16 + count]


def streams_in(refs, layer, rows, n):
    if layer == 0:
        own, oth, n_own, *rest = refs
        keep = slice(REACH, REACH + rows)
        n_oth = carried(oth, n_own.shape[0])
        return own[...].astype(F32)[keep], oth[...].astype(F32)[keep], [n_own, n_oth, *rest]
    own, oth, table, n_own, n_oth, *rest = refs
    keep = slice(REACH, REACH + rows)
    t = table[keep, :]
    s_own = normed(own[keep, :], t, *norm_rows(n_own, layer - 1), n).astype(BF16).astype(F32)
    n_oth = carried(n_oth, n_own.shape[0])
    s_oth = normed(oth[keep, :], t, *norm_rows(n_oth, layer - 1), n).astype(BF16).astype(F32)
    return s_own, s_oth, [n_own, n_oth, *rest]


def layer_body(sc, *refs, n, held, at, layer, scale):
    mixed, refs = refs[:n], refs[n:]
    rows = mixed[0].shape[0]
    own, oth, refs = streams_in(refs, layer, rows, n)
    (n_own, n_oth), w_own, w_oth, refs = take(refs, 2, *held)
    (g_own, b_own), (g_oth, b_oth) = norm_rows(n_own, layer), norm_rows(n_oth, layer)
    outs, (r_own, r_oth, lhs, held_out) = refs[:n], refs[n:]
    own, oth = branch_resid(sc, mixed, own, oth, w_own, w_oth, at, scale)
    r_own[...] = own
    r_oth[...] = oth
    own, oth, mean, second = centred(own, oth)
    width = outs[0].shape[1]
    stats = stat_rows(parts(mean) + parts(second), rows, 2 * width)
    feat = own.shape[1]
    for i, (value, gain, bias) in enumerate(((own, g_own, b_own), (oth, g_oth, b_oth))):
        cols = slice(i * feat, (i + 1) * feat)
        lhs[0:rows, cols] = (value * gain).astype(BF16)
        extra = parts(gain) + parts(bias)
        extra = jnp.concatenate(
            list(extra) + [jnp.zeros((STAT - 6, value.shape[1]), F32)], axis=0
        )
        lhs[rows : rows + STAT, cols] = extra.astype(BF16)
    place = lax.broadcasted_iota(jnp.int32, (STAT, width), 0)

    def project_group(k, carry):
        acc = dot_t(lhs[...], feature_rows(w_own, w_oth, at + 1, (sc[0] + k) % n, n))
        held_out[k, 0:rows, :] = acc[0:rows].astype(BF16)
        tail = acc[rows : rows + STAT]
        sums = parts(tail[0:1] + tail[1:2] + tail[2:3]) + parts(tail[3:4] + tail[4:5] + tail[5:6])
        block = stats[:, width:]
        for i, s in enumerate(sums):
            block = jnp.where(place == 6 + i, s, block)
        held_out[k, rows : rows + STAT, :] = stats[:, :width].astype(BF16)
        held_out[k, rows + STAT :, :] = block.astype(BF16)
        return carry

    lax.fori_loop(0, n, project_group, 0)
    for k in range(n):
        outs[k][...] = held_out[k]


def last_body(sc, *refs, n, held, at, layer, scale):
    mixed, refs = refs[:n], refs[n:]
    rows = mixed[0].shape[0]
    own, oth, refs = streams_in(refs, layer, rows, n)
    _, w_own, w_oth, (r_own, r_oth, stats) = take(refs, 2, *held)
    own, oth = branch_resid(sc, mixed, own, oth, w_own, w_oth, at, scale)
    r_own[...] = own
    r_oth[...] = oth
    _, _, mean, second = centred(own, oth)
    stats[...] = stat_rows((mean, second), rows, stats.shape[1])[0:8]


def finish_body(sc, *refs, width):
    stats, refs = refs[:2], refs[2:]
    r_own, r_oth, n_own, n_oth, out_own, out_oth = refs
    n_oth = carried(n_oth, n_own.shape[0])
    rows = r_own.shape[0]
    rows_of = [(s, i) for s in stats for i in range(0, s.shape[0], 8)]
    means = [s[i : i + 1, :] for s, i in rows_of]
    mean, rstd = combine_stats(means, [s[i + 1 : i + 2, :] for s, i in rows_of], width)
    table = jnp.concatenate([mean, rstd, jnp.zeros((126, mean.shape[1]), F32)], axis=0)
    table = jnp.transpose(table)[0:rows]
    at = pl.ds(pl.multiple_of(sc[3] * rows, 16), rows)
    out_own[at, :] = normed(r_own[...], table, *norm_rows(n_own, n_own.shape[0] // 2 - 1), 0).astype(BF16)
    out_oth[...] = normed(r_oth[...], table, *norm_rows(n_oth, n_oth.shape[0] // 2 - 1), 0).astype(BF16)


def shifted(array, axis, step):
    n = lax.axis_size(axis)
    return lax.ppermute(array, axis, [(i, (i + step) % n) for i in range(n)])


def other(array):
    return lax.ppermute(array, "c", [(0, 1), (1, 0)])


def after(value, *events):
    return lax.optimization_barrier((value, *events))[0]


def over_z(shards):
    spread = jnp.broadcast_to(shards[None], (lax.axis_size("z"), *shards.shape))
    return lax.all_to_all(spread, "z", 0, 0, tiled=True)


def over_y(block):
    return [block] + [shifted(block, "y", k) for k in range(1, lax.axis_size("y"))]


def over_c(own, sizes):
    runs = []
    for size in sizes:
        runs.append(jnp.stack(own[:size]) if size > 1 else own[0][None])
        own = own[size:]
    return runs, [other(b) for b in runs]


def layers_on_device(tokens, in_proj, group_mix, pool_gain, out_proj, norm_gain, norm_bias):
    rows_dev, feat = tokens.shape
    layers = in_proj.shape[0]
    n = lax.axis_size("x")
    sp = lax.axis_size(SP)
    seq_length = rows_dev * sp
    channels = in_proj.shape[2] * sp
    group = channels // n
    half_rows = rows_dev // 2
    pad = layers * REACH
    scale = (2.0 * layers) ** 0.25
    x, c = lax.axis_index("x"), lax.axis_index("c")
    start = lax.axis_index(SP) * rows_dev + c * half_rows

    def scalars(base):
        return jnp.stack([x, base, lax.axis_index("y"), c]).astype(jnp.int32)

    sc = scalars(start)
    ny = lax.axis_size("y")
    sizes = dict(seq_length=seq_length, ny=ny, piece=in_proj.shape[2])
    in_t = jnp.swapaxes(in_proj, 1, 2)
    z_in = over_z(in_t[:1])
    w_in = over_c(over_y(z_in), CORE_RUNS)

    up = [(i, i + 1) for i in range(sp - 1)]
    before = lax.ppermute(tokens[rows_dev - pad :], SP, up)
    behind = lax.ppermute(tokens[:pad], SP, [(j, i) for i, j in up])
    wide = jnp.concatenate([before, tokens, behind], axis=0)
    length = half_rows + 2 * pad
    mine = lax.dynamic_slice_in_dim(wide, c * half_rows, length, 0)
    theirs = lax.dynamic_slice_in_dim(wide, (1 - c) * half_rows, length, 0)
    norm = jnp.concatenate([norm_gain, norm_bias], axis=0)
    rest, tail = norm, []
    for _ in range(3):
        part = lax.reduce_precision(rest, 8, 7)
        tail.append(jnp.pad(part.astype(BF16), ((0, 8 - norm.shape[0]), (0, 0))))
        rest = rest - part
    tail.append(jnp.zeros_like(tail[0]))
    theirs = other(jnp.concatenate([theirs, *tail], axis=0))
    norms = (norm, theirs)

    def block(rows, width, dtype=BF16):
        return jax.ShapeDtypeStruct((rows, width), dtype)

    def exchanged(blocks):
        return [blocks[0]] + [shifted(b, "x", k) for k, b in enumerate(blocks) if k]

    rows = length
    flops = 2 * rows * 2 * feat * channels
    partials = kernel_call(
        functools.partial(project_body, n=n, held=(len(w_in[0]), len(w_in[1]))),
        [block(rows, group)] * n,
        flops=flops,
        scratch=[pltpu.VMEM((n, rows, group), BF16)],
    )(sc, mine, theirs, *w_in[0], *w_in[1])
    stream = [mine, theirs]
    late = [w for l in range(1, layers) for w in (out_proj[l], in_t[min(l + 1, layers - 1)])]
    z_a = over_z(jnp.stack([out_proj[0], in_t[1]]))
    for l in range(layers):
        first, last = l == 0, l == layers - 1
        arrived = exchanged(partials)
        if first:
            y_w = over_y(after(z_a, partials[0]))
        done = rows - 2 * REACH
        here = scalars(start - pad + (l + 1) * REACH)
        mix_flops = 2 * done * group * (rows + group)
        if first:
            mixed = kernel_call(
                functools.partial(mix_first_body, layer=l, **sizes),
                block(done, group),
                flops=mix_flops,
                scratch=[pltpu.VMEM((group, group), BF16), pltpu.SemaphoreType.DMA(())],
                in_hbm=(n + 1,),
            )(here, *arrived, group_mix, pool_gain)
        else:
            mixed, table = kernel_call(
                functools.partial(mix_body, width=2 * feat, layer=l, **sizes),
                [block(done, group), block(rows, 128, F32)],
                flops=mix_flops,
                scratch=[pltpu.VMEM((group, group), BF16), pltpu.SemaphoreType.DMA(())],
                in_hbm=(n + 1,),
            )(here, *arrived, group_mix, pool_gain)
            stream = stream + [table]
        all_mixed = exchanged([mixed] * n)
        if first:
            z_b = over_z(after(jnp.stack(late[:-1]), z_a, partials[0]))
            y_w = lax.optimization_barrier((*y_w, mixed))[:-1]
            own_w, oth_w = over_c(list(y_w), CORE_RUNS)
            y_w = over_y(z_b)
        elif l == 1:
            y_w = lax.optimization_barrier((*y_w, mixed))[:-1]
            own_w, oth_w = over_c(list(y_w), CORE_RUNS)
        held = (len(own_w), len(oth_w))
        at = 2 * max(l - 1, 0)
        rows = done
        resid = [block(rows, feat, F32)] * 2
        if not last:
            *partials, r_own, r_oth = kernel_call(
                functools.partial(layer_body, n=n, held=held, at=at, layer=l, scale=scale),
                [block(rows + 2 * STAT, group)] * n + resid,
                scratch=[
                    pltpu.VMEM((rows + STAT, 2 * feat), BF16),
                    pltpu.VMEM((n, rows + 2 * STAT, group), BF16),
                ],
                flops=4 * rows * 2 * feat * channels,
                limit=LIMITS[l],
            )(here, *all_mixed, *stream, *(norms[:1] if first else norms), *own_w, *oth_w)
            stream = [r_own, r_oth]
        else:
            r_own, r_oth, stats = kernel_call(
                functools.partial(last_body, n=n, held=held, at=at, layer=l, scale=scale),
                resid + [block(8, rows, F32)],
                flops=2 * rows * 2 * feat * channels,
            )(here, *all_mixed, *stream, *(norms[:1] if first else norms), *own_w, *oth_w)
            near = lax.ppermute(stats, "x", [(i, i ^ 1) for i in range(n)])
            stats = jnp.concatenate([stats, near], axis=0)
            far = lax.ppermute(stats, "x", [(i, i ^ 2) for i in range(n)])
            out_own, out_oth = kernel_call(
                functools.partial(finish_body, width=2 * feat),
                [block(rows_dev, feat), block(rows, feat)],
            )(here, stats, far, r_own, r_oth, *norms)
    return lax.dynamic_update_slice_in_dim(out_own, other(out_oth), (1 - c) * half_rows, 0)


def solution(mesh):
    split = Mesh(mesh.devices.reshape(8, 4, 4, 2), ("z", "y", "x", "c"))
    tp = ("x", "c")
    in_specs = (P(SP, tp), P(None, tp, SP), P(), P(), P(None, SP, tp), P(None, tp), P(None, tp))
    return jax.shard_map(
        layers_on_device, mesh=split, in_specs=in_specs, out_specs=P(SP, tp), check_vma=False
    )
```

```python
import functools

import jax
import jax.numpy as jnp
from jax import lax
from jax.experimental import pallas as pl
from jax.experimental.pallas import tpu as pltpu
from jax.sharding import Mesh
from jax.sharding import PartitionSpec as P


SP = ("z", "y")
norm_eps = 1e-05
REACH = 8
STAT = 16
F32, BF16 = jnp.float32, jnp.bfloat16
CORE_RUNS = (2, 2)
LIMITS = (60 * 2**20, 20 * 2**20)
VMEM_LIMIT = 20 * 2**20


def nbytes(shapes):
    return sum(s.size * s.dtype.itemsize for s in shapes)


def kernel_call(body, out_shape, scratch=(), flops=0, limit=VMEM_LIMIT, in_hbm=()):
    def call(*args):
        outs = out_shape if isinstance(out_shape, (list, tuple)) else [out_shape]
        specs = [pl.BlockSpec(memory_space=pltpu.SMEM)]
        specs += [
            pl.BlockSpec(memory_space=pl.ANY if i in in_hbm else pltpu.VMEM)
            for i in range(1, len(args))
        ]
        return pl.pallas_call(
            body,
            out_shape=out_shape,
            in_specs=specs,
            scratch_shapes=list(scratch),
            compiler_params=pltpu.CompilerParams(vmem_limit_bytes=limit),
            cost_estimate=pl.CostEstimate(
                flops=flops, bytes_accessed=nbytes(args) + nbytes(outs), transcendentals=0
            ),
        )(*args)

    return call


def dot(a, b):
    return lax.dot_general(a, b, (((1,), (0,)), ((), ())), preferred_element_type=F32)


def dot_t(a, b):
    return lax.dot_general(a, b, (((1,), (1,)), ((), ())), preferred_element_type=F32)


def parts(v):
    hi = v.astype(BF16).astype(F32)
    mid = (v - hi).astype(BF16).astype(F32)
    low = (v - hi - mid).astype(BF16).astype(F32)
    return hi, mid, low


def group_rows(weights, m, g, n):
    per = weights[0].shape[1] // n
    rows = [
        w[k, g * per + z, m] for z in range(per) for w in weights for k in range(w.shape[0])
    ]
    return jnp.concatenate(rows, axis=0)


def feature_rows(own, oth, m, g, n):
    return jnp.concatenate([group_rows(own, m, g, n), group_rows(oth, m, g, n)], axis=1)


def take(refs, *counts):
    out = []
    for m in counts:
        out.append(refs[:m])
        refs = refs[m:]
    return *out, refs


def spread(held, outs):
    rows = held.shape[1]
    size = max(m for m in range(16, 97, 16) if rows % m == 0)

    def copy(i, carry):
        at = pl.ds(pl.multiple_of(i * size, 16), size)
        for k, out in enumerate(outs):
            out[at, :] = held[k, at, :]
        return carry

    lax.fori_loop(0, rows // size, copy, 0)


def project_body(sc, own, oth, *refs, n, held):
    w_own, w_oth, (*outs, held_out) = take(refs, *held)

    def project_group(k, carry):
        both = jnp.concatenate([own[...], oth[...]], axis=1)
        acc = dot_t(both, feature_rows(w_own, w_oth, 0, (sc[0] + k) % n, n))
        held_out[k] = acc.astype(BF16)
        return carry

    lax.fori_loop(0, n, project_group, 0)
    spread(held_out, outs)


def pooled_mix(sc, proj, fetch, group_map, gains, out, layer, seq_length, ny, piece):
    rows_in, rows_out = proj.shape[0], out.shape[0]
    half = lax.shift_left(jnp.int32(1), sc[0])
    base = sc[1]
    col = lax.broadcasted_iota(jnp.int32, (rows_out, rows_in), 1) - REACH
    at = lax.broadcasted_iota(jnp.int32, (rows_out, 1), 0)
    low = jnp.maximum(at - half, -base)
    high = jnp.minimum(at + half, seq_length - base)
    band = jnp.where((col >= low) & (col < high), 1.0, 0.0).astype(BF16)
    count = jnp.maximum(high - low, 1).astype(F32)
    centre = proj.astype(F32)[REACH : REACH + rows_out]
    differ = (dot(band, proj) / count - centre).astype(BF16)
    width = proj.shape[1]
    true = lax.broadcasted_iota(jnp.int32, (width, width), 0)
    held = lax.broadcasted_iota(jnp.int32, (width, width), 1)
    z, k, i = held // (ny * piece), (held // piece) % ny, held % piece
    turn = jnp.where(true == (z * ny + (sc[2] + ny - k) % ny) * piece + i, 1.0, 0.0).astype(BF16)
    differ = dot_t(differ, turn).astype(BF16)
    gain = gains[layer : layer + 1, 0:width]
    for g in range(1, gains.shape[1] // width):
        gain = jnp.where(sc[0] == g, gains[layer : layer + 1, g * width : (g + 1) * width], gain)
    fetch.wait()
    mixed = (dot(differ, group_map[...]) * gain).astype(BF16)
    out[...] = dot(mixed, turn).astype(BF16)


def mix_first_body(sc, *refs, **sizes):
    *partials, maps, gains, out, group_map, sem = refs
    fetch = pltpu.make_async_copy(maps.at[sizes["layer"], sc[0]], group_map, sem)
    fetch.start()
    total = partials[0][...].astype(F32)
    for p in partials[1:]:
        total = total + p[...].astype(F32)
    pooled_mix(sc, total.astype(BF16), fetch, group_map, gains, out, **sizes)


def combine_stats(means, seconds, width):
    n = len(means)
    mean = means[0]
    for m in means[1:]:
        mean = mean + m
    mean = mean / n
    second = seconds[0] + width * jnp.square(means[0] - mean)
    for m, s in zip(means[1:], seconds[1:]):
        second = second + s + width * jnp.square(m - mean)
    return mean, lax.rsqrt(second / (n * width) + norm_eps)


def mix_body(sc, *refs, width, **sizes):
    *partials, maps, gains, out, row_out, group_map, sem = refs
    fetch = pltpu.make_async_copy(maps.at[sizes["layer"], sc[0]], group_map, sem)
    fetch.start()
    n = len(partials)
    rows = partials[0].shape[0] - 2 * STAT
    means, seconds, gw = [], [], []
    total, bw = None, None
    for p in partials:
        stat = jnp.concatenate(
            [p[rows : rows + STAT, :].astype(F32), p[rows + STAT :, :].astype(F32)], axis=1
        )
        means.append(stat[0:1] + stat[1:2] + stat[2:3])
        seconds.append(stat[3:4] + stat[4:5] + stat[5:6])
        chan = p[rows + STAT :, :].astype(F32)
        gw.append(chan[6:7] + chan[7:8] + chan[8:9])
        b = chan[9:10] + chan[10:11] + chan[11:12]
        bw = b if bw is None else bw + b
        q = p[0:rows, :].astype(F32)
        total = q if total is None else total + q
    mean, rstd = combine_stats(means, seconds, width)
    table = jnp.concatenate(
        [m - mean for m in means] + [mean, rstd, jnp.zeros((126 - n, mean.shape[1]), F32)], axis=0
    )
    table = jnp.transpose(table)[0:rows]
    row_out[...] = table
    for k in range(n):
        total = total + table[:, k : k + 1] * gw[k]
    proj = (total * table[:, n + 1 : n + 2] + bw).astype(BF16)
    pooled_mix(sc, proj, fetch, group_map, gains, out, **sizes)


def normed(resid, table, gain, bias, n):
    return (resid - table[:, n : n + 1]) * table[:, n + 1 : n + 2] * gain + bias


def branch_resid(sc, mixed, own, oth, w_own, w_oth, m, scale):
    n = len(mixed)
    block = jnp.concatenate([b[...] for b in mixed], axis=1)
    order = [(sc[0] + n - k) % n for k in range(n)]

    def branch(weights):
        return dot(block, jnp.concatenate([group_rows(weights, m, g, n) for g in order], axis=0))

    return scale * own + branch(w_own), scale * oth + branch(w_oth)


def centred(own, oth):
    width = own.shape[1] + oth.shape[1]
    mean = (jnp.sum(own, 1, keepdims=True) + jnp.sum(oth, 1, keepdims=True)) / width
    own, oth = own - mean, oth - mean
    second = jnp.sum(own * own, 1, keepdims=True) + jnp.sum(oth * oth, 1, keepdims=True)
    return own, oth, mean, second


def stat_rows(columns, rows, lanes):
    place = lax.broadcasted_iota(jnp.int32, (rows, 128), 1)
    table = jnp.zeros((rows, 128), F32)
    for i, c in enumerate(columns):
        table = jnp.where(place == i, c, table)
    if lanes > rows:
        table = jnp.concatenate([table, jnp.zeros((lanes - rows, 128), F32)], axis=0)
    return jnp.transpose(table)[0:STAT]


def norm_rows(norm, layer):
    layers = norm.shape[0] // 2
    return norm[layer : layer + 1, :], norm[layers + layer : layers + layer + 1, :]


def streams_in(refs, layer, rows, n):
    if layer == 0:
        own, oth, *rest = refs
        keep = slice(REACH, REACH + rows)
        return own[...].astype(F32)[keep], oth[...].astype(F32)[keep], rest
    own, oth, table, n_own, n_oth, *rest = refs
    keep = slice(REACH, REACH + rows)
    t = table[keep, :]
    s_own = normed(own[keep, :], t, *norm_rows(n_own, layer - 1), n).astype(BF16).astype(F32)
    s_oth = normed(oth[keep, :], t, *norm_rows(n_oth, layer - 1), n).astype(BF16).astype(F32)
    return s_own, s_oth, [n_own, n_oth, *rest]


def layer_body(sc, *refs, n, held, at, layer, scale):
    mixed, refs = refs[:n], refs[n:]
    rows = mixed[0].shape[0]
    own, oth, refs = streams_in(refs, layer, rows, n)
    (n_own, n_oth), w_own, w_oth, refs = take(refs, 2, *held)
    (g_own, b_own), (g_oth, b_oth) = norm_rows(n_own, layer), norm_rows(n_oth, layer)
    outs, (r_own, r_oth, lhs, held_out) = refs[:n], refs[n:]
    own, oth = branch_resid(sc, mixed, own, oth, w_own, w_oth, at, scale)
    r_own[...] = own
    r_oth[...] = oth
    own, oth, mean, second = centred(own, oth)
    width = outs[0].shape[1]
    stats = stat_rows(parts(mean) + parts(second), rows, 2 * width)
    feat = own.shape[1]
    for i, (value, gain, bias) in enumerate(((own, g_own, b_own), (oth, g_oth, b_oth))):
        cols = slice(i * feat, (i + 1) * feat)
        lhs[0:rows, cols] = (value * gain).astype(BF16)
        extra = parts(gain) + parts(bias)
        extra = jnp.concatenate(
            list(extra) + [jnp.zeros((STAT - 6, value.shape[1]), F32)], axis=0
        )
        lhs[rows : rows + STAT, cols] = extra.astype(BF16)
    place = lax.broadcasted_iota(jnp.int32, (STAT, width), 0)

    def project_group(k, carry):
        acc = dot_t(lhs[...], feature_rows(w_own, w_oth, at + 1, (sc[0] + k) % n, n))
        held_out[k, 0:rows, :] = acc[0:rows].astype(BF16)
        tail = acc[rows : rows + STAT]
        sums = parts(tail[0:1] + tail[1:2] + tail[2:3]) + parts(tail[3:4] + tail[4:5] + tail[5:6])
        block = stats[:, width:]
        for i, s in enumerate(sums):
            block = jnp.where(place == 6 + i, s, block)
        held_out[k, rows : rows + STAT, :] = stats[:, :width].astype(BF16)
        held_out[k, rows + STAT :, :] = block.astype(BF16)
        return carry

    lax.fori_loop(0, n, project_group, 0)
    spread(held_out, outs)


def last_body(sc, *refs, n, held, at, layer, scale):
    mixed, refs = refs[:n], refs[n:]
    rows = mixed[0].shape[0]
    own, oth, refs = streams_in(refs, layer, rows, n)
    _, w_own, w_oth, (r_own, r_oth, stats) = take(refs, 2, *held)
    own, oth = branch_resid(sc, mixed, own, oth, w_own, w_oth, at, scale)
    r_own[...] = own
    r_oth[...] = oth
    _, _, mean, second = centred(own, oth)
    stats[...] = stat_rows((mean, second), rows, stats.shape[1])[0:8]


def finish_body(sc, *refs, n, width):
    stats, refs = refs[:n], refs[n:]
    r_own, r_oth, n_own, n_oth, out_own, out_oth = refs
    rows = r_own.shape[0]
    mean, rstd = combine_stats([s[0:1, :] for s in stats], [s[1:2, :] for s in stats], width)
    table = jnp.concatenate([mean, rstd, jnp.zeros((126, mean.shape[1]), F32)], axis=0)
    table = jnp.transpose(table)[0:rows]
    at = pl.ds(pl.multiple_of(sc[3] * rows, 16), rows)
    out_own[at, :] = normed(r_own[...], table, *norm_rows(n_own, n_own.shape[0] // 2 - 1), 0).astype(BF16)
    out_oth[...] = normed(r_oth[...], table, *norm_rows(n_oth, n_oth.shape[0] // 2 - 1), 0).astype(BF16)


def shifted(array, axis, step):
    n = lax.axis_size(axis)
    return lax.ppermute(array, axis, [(i, (i + step) % n) for i in range(n)])


def other(array):
    return lax.ppermute(array, "c", [(0, 1), (1, 0)])


def after(value, *events):
    return lax.optimization_barrier((value, *events))[0]


def over_z(shards):
    spread = jnp.broadcast_to(shards[None], (lax.axis_size("z"), *shards.shape))
    return lax.all_to_all(spread, "z", 0, 0, tiled=True)


def over_y(block):
    return [block] + [shifted(block, "y", k) for k in range(1, lax.axis_size("y"))]


def over_c(own, sizes, event=None):
    runs, swapped = [], []
    for size in sizes:
        now = own[:size]
        if event is not None:
            now = lax.optimization_barrier((*now, event))[:-1]
        event = jnp.stack(now) if size > 1 else now[0][None]
        runs.append(event)
        swapped.append(other(event))
        own = own[size:]
    return runs, swapped


def layers_on_device(tokens, in_proj, group_mix, pool_gain, out_proj, norm_gain, norm_bias):
    rows_dev, feat = tokens.shape
    layers = in_proj.shape[0]
    n = lax.axis_size("x")
    sp = lax.axis_size(SP)
    seq_length = rows_dev * sp
    channels = in_proj.shape[2] * sp
    group = channels // n
    half_rows = rows_dev // 2
    pad = layers * REACH
    scale = (2.0 * layers) ** 0.25
    x, c = lax.axis_index("x"), lax.axis_index("c")
    start = lax.axis_index(SP) * rows_dev + c * half_rows

    def scalars(base):
        return jnp.stack([x, base, lax.axis_index("y"), c]).astype(jnp.int32)

    sc = scalars(start)
    ny = lax.axis_size("y")
    sizes = dict(seq_length=seq_length, ny=ny, piece=in_proj.shape[2])
    first_in = jnp.swapaxes(in_proj[:1], 1, 2)
    in_t = [None, *jnp.swapaxes(after(in_proj[1:], first_in), 1, 2)]
    z_in = over_z(first_in)
    w_in = over_c(over_y(z_in), CORE_RUNS)

    up = [(i, i + 1) for i in range(sp - 1)]
    before = lax.ppermute(tokens[rows_dev - pad :], SP, up)
    behind = lax.ppermute(tokens[:pad], SP, [(j, i) for i, j in up])
    wide = jnp.concatenate([before, tokens, behind], axis=0)
    length = half_rows + 2 * pad
    mine = lax.dynamic_slice_in_dim(wide, c * half_rows, length, 0)
    theirs = other(lax.dynamic_slice_in_dim(wide, (1 - c) * half_rows, length, 0))
    norm = jnp.concatenate([norm_gain, norm_bias], axis=0)
    norms = (norm, other(norm))
    mine = after(mine, norms[1])

    def block(rows, width, dtype=BF16):
        return jax.ShapeDtypeStruct((rows, width), dtype)

    def exchanged(blocks):
        return [blocks[0]] + [shifted(b, "x", k) for k, b in enumerate(blocks) if k]

    rows = length
    flops = 2 * rows * 2 * feat * channels
    partials = kernel_call(
        functools.partial(project_body, n=n, held=(len(w_in[0]), len(w_in[1]))),
        [block(rows, group)] * n,
        flops=flops,
        scratch=[pltpu.VMEM((n, rows, group), BF16)],
    )(sc, mine, theirs, *w_in[0], *w_in[1])
    stream = [mine, theirs]
    late = [w for l in range(1, layers) for w in (out_proj[l], in_t[min(l + 1, layers - 1)])]
    z_a = over_z(jnp.stack([out_proj[0], in_t[1]]))
    for l in range(layers):
        first, last = l == 0, l == layers - 1
        arrived = exchanged(partials)
        if first:
            y_w = over_y(after(z_a, partials[0]))
        done = rows - 2 * REACH
        here = scalars(start - pad + (l + 1) * REACH)
        mix_flops = 2 * done * group * (rows + group)
        if first:
            mixed = kernel_call(
                functools.partial(mix_first_body, layer=l, **sizes),
                block(done, group),
                flops=mix_flops,
                scratch=[pltpu.VMEM((group, group), BF16), pltpu.SemaphoreType.DMA(())],
                in_hbm=(n + 1,),
            )(here, *arrived, group_mix, pool_gain)
        else:
            mixed, table = kernel_call(
                functools.partial(mix_body, width=2 * feat, layer=l, **sizes),
                [block(done, group), block(rows, 128, F32)],
                flops=mix_flops,
                scratch=[pltpu.VMEM((group, group), BF16), pltpu.SemaphoreType.DMA(())],
                in_hbm=(n + 1,),
            )(here, *arrived, group_mix, pool_gain)
            stream = stream + [table]
        all_mixed = exchanged([mixed] * n)
        if first:
            z_b = over_z(jnp.stack(late[:-1]))
            own_w, oth_w = over_c(y_w, CORE_RUNS, mixed)
            y_w = over_y(z_b)
        elif l == 1:
            own_w, oth_w = over_c(y_w, (ny,), mixed)
        held = (len(own_w), len(oth_w))
        at = 2 * max(l - 1, 0)
        rows = done
        resid = [block(rows, feat, F32)] * 2
        if not last:
            *partials, r_own, r_oth = kernel_call(
                functools.partial(layer_body, n=n, held=held, at=at, layer=l, scale=scale),
                [block(rows + 2 * STAT, group)] * n + resid,
                scratch=[
                    pltpu.VMEM((rows + STAT, 2 * feat), BF16),
                    pltpu.VMEM((n, rows + 2 * STAT, group), BF16),
                ],
                flops=4 * rows * 2 * feat * channels,
                limit=LIMITS[l],
            )(here, *all_mixed, *stream, *norms, *own_w, *oth_w)
            stream = [r_own, r_oth]
        else:
            r_own, r_oth, stats = kernel_call(
                functools.partial(last_body, n=n, held=held, at=at, layer=l, scale=scale),
                resid + [block(8, rows, F32)],
                flops=2 * rows * 2 * feat * channels,
            )(here, *all_mixed, *stream, *norms, *own_w, *oth_w)
            out_own, out_oth = kernel_call(
                functools.partial(finish_body, n=n, width=2 * feat),
                [block(rows_dev, feat), block(rows, feat)],
            )(here, *exchanged([stats] * n), r_own, r_oth, *norms)
    return lax.dynamic_update_slice_in_dim(out_own, other(out_oth), (1 - c) * half_rows, 0)


def solution(mesh):
    split = Mesh(mesh.devices.reshape(8, 4, 4, 2), ("z", "y", "x", "c"))
    tp = ("x", "c")
    in_specs = (P(SP, tp), P(None, tp, SP), P(), P(), P(None, SP, tp), P(None, tp), P(None, tp))
    return jax.shard_map(
        layers_on_device, mesh=split, in_specs=in_specs, out_specs=P(SP, tp), check_vma=False
    )
```
